32 devices in a mesh: grp: 2 (over y), sp: 4 (over z), tp: 4 (over x, core).
Axes of the slice: x: 2, y: 2, z: 4, core: 2. Of those that a mesh axis runs over, the one named last changes fastest.
Arguments:
- query_rows: bfloat16 [4096, 512], P(('grp', 'sp'), 'tp'), parts along dimension 0, may hold values from -12 to 12
- key_rows: bfloat16 [4096, 512], P(('grp', 'sp'), 'tp'), parts along dimension 0, may hold values from -12 to 12
- value_rows: bfloat16 [4096, 512], P(('grp', 'sp'), 'tp'), parts along dimension 0, may hold values from -12 to 12
- residual: bfloat16 [4096, 2048], P(('grp', 'sp', 'tp')), parts along dimension 0, may hold values from -6 to 6
- output_weight: bfloat16 [512, 2048], P('tp'), may hold values from -0.25 to 0.25
- first_gain: float32 [2048], replicated, may hold values from 0.1 to 1.9
- first_bias: float32 [2048], replicated, may hold values from -3 to 3
- expert_ids: int32 [4096, 4], P(('grp', 'sp', 'tp')), parts along dimension 0, may hold values from 0 to 15, all different within a row; in each aligned block of 128 rows (0 to 127, 128 to 255, ...) at most 48 rows name the same one
- expert_share: float32 [4096, 4], P(('grp', 'sp', 'tp')), parts along dimension 0, may hold values from 0.3 to 1.2
- gate_weight: bfloat16 [16, 2048, 256], P(('sp', 'tp')), may hold values from -0.125 to 0.125
- up_weight: bfloat16 [16, 2048, 256], P(('sp', 'tp')), may hold values from -0.125 to 0.125
- down_weight: bfloat16 [16, 256, 2048], P(('sp', 'tp')), may hold values from -0.375 to 0.375
- shared_gate: bfloat16 [2048, 512], replicated, may hold values from -0.125 to 0.125
- shared_up: bfloat16 [2048, 512], replicated, may hold values from -0.125 to 0.125
- shared_down: bfloat16 [512, 2048], replicated, may hold values from -0.25 to 0.25
- second_gain: float32 [2048], replicated, may hold values from 0.1 to 1.9
- second_bias: float32 [2048], replicated, may hold values from -3 to 3
Outputs:
- layer_out: bfloat16 [4096, 2048], P(('grp', 'sp', 'tp')), parts along dimension 0
The draws below stay inside these ranges and needn't reach their ends.
There are 2 independent parts, one for each index of `grp`. The reference program is written for one: setup_inputs(seed, part) draws one part's arguments, and reference() takes and returns one part's arrays. A program takes and returns all parts, laid end to end along the dimension named above; an argument that names none is the same for every part. Nothing has to cross between parts.
Inputs may be any that keep to these rules, and one draw needn't show every extreme that they name: `expert_ids`: each row names 4 different experts. Among the rows of one device (aligned blocks of 128 rows) no expert is named by more than 48 rows, a bound that some block reaches.
All inputs are finite; a program needn't handle non-finite values.
Results may differ from the reference program's by a relative error of at most 0.012.
Values may be sent and summed in bfloat16 or wider, within the bound.
A program may use at most 128 MiB of HBM per device.

```python
import math
import jax
import jax.numpy as jnp
import numpy as np
from jax import lax

HEADS = 4
HEAD_DIM = 128
D = 2048
EFF = 256
SFF = 512
TOP_K = 4
KBLK = 128
T_SP = 512
TOK = 128
SEQUENCE_LENGTH = 2048
QH = 512
EXPERTS = 16
CAP = 48


def head_plan(key):
    baseline_value = jax.random.fold_in(key, 101)
    direction_key, selection_key, quick_rate_key, gentle_rate_key, multiplier_key, spike_event_key = jax.random.split(baseline_value, 6)
    directions = jax.random.normal(direction_key, (HEADS, HEAD_DIM), jnp.float32)
    directions = directions / jnp.sqrt(jnp.sum(directions * directions, axis=1, keepdims=True))
    slow_share = 0.5
    is_slow = jax.random.uniform(selection_key, (HEADS,), jnp.float32) < slow_share
    fast_rate = jax.random.uniform(quick_rate_key, (HEADS,), jnp.float32, 2.5, 3.8)
    slow_rate = math.log(SEQUENCE_LENGTH) + 1.0 + jax.random.uniform(gentle_rate_key, (HEADS,), jnp.float32, 0.0, 0.4)
    rates = jnp.where(is_slow, slow_rate, fast_rate)
    factors = jnp.exp(jax.random.uniform(multiplier_key, (SEQUENCE_LENGTH // KBLK, HEADS), jnp.float32, -0.15, 0.15))
    position_indices = jnp.arange(SEQUENCE_LENGTH)
    coefs = factors[position_indices // KBLK]
    spike_events = jax.random.randint(spike_event_key, (3,), 0, SEQUENCE_LENGTH)
    spike_hits = jnp.any(position_indices[:, None] == spike_events[None, :], axis=1)
    coefs = jnp.where(spike_hits[:, None], 1.2 / rates[None, :], coefs)
    return (directions, rates, coefs)


def noise_for(key):
    noise = 0.5 * jax.random.normal(key, (SEQUENCE_LENGTH, HEADS, HEAD_DIM), jnp.float32)
    return noise


def draw_query_rows(key, part):
    directions, rates, coefs = head_plan(key)
    amps = jnp.sqrt(rates) * HEAD_DIM ** 0.25
    noise = noise_for(jax.random.fold_in(key, 211))
    rows = noise - amps[None, :, None] * directions[None, :, :]
    return jnp.clip(rows.reshape(SEQUENCE_LENGTH, QH), -12.0, 12.0).astype(jnp.bfloat16)


def draw_key_rows(key, part):
    directions, rates, coefs = head_plan(key)
    amps = jnp.sqrt(rates) * HEAD_DIM ** 0.25
    noise = noise_for(jax.random.fold_in(key, 223))
    rows = noise + (coefs * amps[None, :])[:, :, None] * directions[None, :, :]
    return jnp.clip(rows.reshape(SEQUENCE_LENGTH, QH), -12.0, 12.0).astype(jnp.bfloat16)


def draw_value_rows(key, part):
    key_noise = jax.random.fold_in(key, 227)
    key_offset = jax.random.fold_in(key, 229)
    noise = jax.random.normal(key_noise, (SEQUENCE_LENGTH, HEADS, HEAD_DIM), jnp.float32)
    offsets = jax.random.normal(key_offset, (16, HEADS, HEAD_DIM), jnp.float32)
    region = jnp.arange(SEQUENCE_LENGTH) * 16 // SEQUENCE_LENGTH
    rows = noise + offsets[region]
    return jnp.clip(rows.reshape(SEQUENCE_LENGTH, QH), -12.0, 12.0).astype(jnp.bfloat16)


def block_levels(own_key, shape, cuts, low, largest):
    def one(dim, blocks):
        draws = jax.random.uniform(jax.random.fold_in(jax.random.fold_in(own_key, 6), dim), (blocks,), jnp.float32, low / len(cuts), largest / len(cuts))
        return jnp.repeat(jnp.exp(draws), shape[dim] // blocks).reshape((-1,) + (1,) * (len(shape) - dim - 1))

    level = one(*cuts[0])
    for cut in cuts[1:]:
        level = level * one(*cut)
    return level


def routed_block(own_key, own, number, rows, amount, top, most, skew):
    order = jax.random.permutation(own_key, amount)
    crowded, usual = load_shares(amount, rows * top, most, skew, True), load_shares(amount, rows * top, most, skew, False)
    places = jnp.arange(amount)

    def named(sizes, rotation):
        used = int((sizes > 0).sum())
        fixed = max(1, used // 4)
        moved = fixed + (places - fixed + rotation * (used - fixed)) % max(1, amount - fixed)
        return jnp.zeros((amount,), jnp.int32).at[order[jnp.where(places < fixed, places, moved)]].set(jnp.asarray(sizes, jnp.int32))

    sizes = jnp.where(number % 4 == 0, named(crowded, number // 4), named(usual, number - number // 4 - 1))
    mixed = jax.random.permutation(jax.random.fold_in(own, 3), amount)
    source_of, taker = mixed[0:amount // 2 * 2:2], mixed[1:amount // 2 * 2:2]
    slack = jnp.minimum(sizes[source_of] - 1, most - sizes[taker]) // 2
    slack = jnp.where((source_of == order[0]) | (taker == order[0]) | (sizes[taker] == 0), 0, jnp.maximum(slack, 0))
    moved = jax.random.randint(jax.random.fold_in(own, 4), (amount // 2,), 0, 1 << 20) % (slack + 1)
    sizes = sizes.at[source_of].add(-moved).at[taker].add(moved)
    items = jnp.searchsorted(jnp.cumsum(sizes), jnp.arange(rows * top), side="right").astype(jnp.int32)
    listing = items.reshape(top, rows).T
    listing = listing[jax.random.permutation(jax.random.fold_in(own, 1), rows)]
    rotation = jax.random.randint(jax.random.fold_in(own, 2), (rows, 1), 0, top)
    return jnp.take_along_axis(listing, (jnp.arange(top)[None, :] + rotation) % top, axis=1)


def load_shares(number_of, total, reach, slope, full):
    loads = [(1 << 20) // math.isqrt(grade ** slope) + 1 for grade in range(1, number_of + 1)]
    largest = reach if full else min(reach, max(-(-total // number_of), total * loads[0] // sum(loads)))
    least = 1 if total - largest >= number_of - 1 else 0
    holding, rest = [largest] + [least] * (number_of - 1), total - largest - least * (number_of - 1)
    while rest > 0:
        candidates = [i for i in range(1, number_of) if holding[i] < largest] or [i for i in range(1, number_of) if holding[i] < reach]
        pool, budget = sum([loads[i] for i in candidates]), rest
        for i in candidates:
            extra = min(reach - holding[i], max(1, budget * loads[i] // pool), rest)
            holding[i] = holding[i] + extra
            rest = rest - extra
    return np.array(holding)


def normal_values(rng, shape, deviation, limit, cuts=(), kind=jnp.bfloat16):
    values = jax.random.normal(rng, shape, jnp.float32) * deviation
    if len(cuts) > 0:
        values = block_levels(rng, shape, cuts, -0.22, 0.18) * values
    return jnp.clip(values, min=-limit, max=limit).astype(kind)


def setup_inputs(seed: int = 0, part: int = 0) -> dict:
    splits = jax.random.split(jax.random.key(seed), 18)
    part_keys = jax.random.split(jax.random.fold_in(splits[17], part), 18)
    query_rows = draw_query_rows(jax.random.fold_in(jax.random.fold_in(splits[17], part), 71), part)
    key_rows = draw_key_rows(jax.random.fold_in(jax.random.fold_in(splits[17], part), 71), part)
    value_rows = draw_value_rows(jax.random.fold_in(jax.random.fold_in(splits[17], part), 71), part)
    residual = normal_values(part_keys[3], (SEQUENCE_LENGTH, D), 1.0, 6.0, ((0, 16),))
    output_weight = normal_values(splits[4], (QH, D), QH ** -0.5, 0.25, ((0, 4),))
    first_gain = jnp.clip(1.0 + 0.18 * jax.random.normal(splits[5], (D,), jnp.float32), 0.1, 1.9)
    first_bias = normal_values(splits[6], (D,), 0.5, 3.0, (), jnp.float32)
    expert_ids_keys = jax.random.split(jax.random.fold_in(part_keys[7], 1), SEQUENCE_LENGTH // TOK)
    expert_ids_turns = jax.random.permutation(jax.random.fold_in(part_keys[7], 3), SEQUENCE_LENGTH // TOK)
    expert_ids = jax.vmap(lambda own, number: routed_block(jax.random.fold_in(part_keys[7], 2), own, number, TOK, EXPERTS, TOP_K, CAP, 1))(expert_ids_keys, expert_ids_turns).reshape((SEQUENCE_LENGTH, TOP_K))
    expert_share = jnp.clip(jnp.exp(math.log(1.2) - 1.3862944 * jax.random.uniform(part_keys[8], (SEQUENCE_LENGTH, TOP_K), jnp.float32) ** block_levels(part_keys[8], (SEQUENCE_LENGTH, TOP_K), ((0, 16),), -0.2, 0.2)), 0.3, 1.2)
    gate_weight = normal_values(splits[9], (EXPERTS, D, EFF), D ** -0.5, 0.125, ((0, 16),))
    up_weight = normal_values(splits[10], (EXPERTS, D, EFF), D ** -0.5, 0.125, ((0, 16),))
    down_weight = normal_values(splits[11], (EXPERTS, EFF, D), EFF ** -0.5, 0.375, ((0, 16),))
    shared_gate = normal_values(splits[12], (D, SFF), D ** -0.5, 0.125)
    shared_up = normal_values(splits[13], (D, SFF), D ** -0.5, 0.125)
    shared_down = normal_values(splits[14], (SFF, D), SFF ** -0.5, 0.25)
    second_gain = jnp.clip(1.0 + 0.18 * jax.random.normal(splits[15], (D,), jnp.float32), 0.1, 1.9)
    second_bias = normal_values(splits[16], (D,), 0.5, 3.0, (), jnp.float32)
    return {"query_rows": query_rows, "key_rows": key_rows, "value_rows": value_rows, "residual": residual, "output_weight": output_weight, "first_gain": first_gain, "first_bias": first_bias, "expert_ids": expert_ids, "expert_share": expert_share, "gate_weight": gate_weight, "up_weight": up_weight, "down_weight": down_weight, "shared_gate": shared_gate, "shared_up": shared_up, "shared_down": shared_down, "second_gain": second_gain, "second_bias": second_bias}


NORM_EPS = 1e-05

def layer_norm(summed, gains, offset):
    average = lax.optimization_barrier(jnp.mean(summed, axis=-1, keepdims=True))
    centred = summed - average
    spread = lax.optimization_barrier(jnp.mean(centred * centred, axis=-1, keepdims=True))
    return centred * lax.rsqrt(spread + NORM_EPS) * gains.astype(jnp.float32) + offset.astype(jnp.float32)

def stick_attention(query_rows, key_rows, value_rows):
    scale = HEAD_DIM ** (-0.5)
    queries = query_rows.astype(jnp.float32).reshape(SEQUENCE_LENGTH // T_SP, T_SP, HEADS, HEAD_DIM)
    keys = key_rows.astype(jnp.float32).reshape(SEQUENCE_LENGTH // KBLK, KBLK, HEADS, HEAD_DIM)
    values = value_rows.astype(jnp.float32).reshape(SEQUENCE_LENGTH // KBLK, KBLK, HEADS, HEAD_DIM)

    def one_block(packed):
        query_block, which = packed
        query_pos = which * T_SP + jnp.arange(T_SP, dtype=jnp.int32)
        visits = (which + 1) * (T_SP // KBLK)

        def visit(visit_no, carry):
            summed, behind = carry
            chosen = visits - 1 - visit_no
            key_block = lax.dynamic_index_in_dim(keys, chosen, 0, keepdims=False)
            value_block = lax.dynamic_index_in_dim(values, chosen, 0, keepdims=False)
            key_pos = chosen * KBLK + jnp.arange(KBLK, dtype=jnp.int32)
            score = jnp.einsum('qhd,khd->qhk', query_block, key_block) * scale
            usable = key_pos[None, None, :] < query_pos[:, None, None]
            spent = jnp.where(usable, jax.nn.softplus(score), 0.0)
            running = jnp.cumsum(spent, axis=-1)
            totals = running[..., -1]
            inside = totals[..., None] - running + spent
            weight = jnp.where(usable, jnp.exp(score - inside), 0.0)
            weight = lax.optimization_barrier(weight.astype(jnp.bfloat16)).astype(jnp.float32)
            pieces = jnp.einsum('qhk,khd->qhd', weight, value_block)
            summed = summed + pieces * jnp.exp(-behind)[..., None]
            return (summed, behind + totals)
        initial = (jnp.zeros((T_SP, HEADS, HEAD_DIM), jnp.float32), jnp.zeros((T_SP, HEADS), jnp.float32))
        summed, _ = lax.fori_loop(0, visits, visit, initial)
        return summed.reshape(T_SP, QH).astype(jnp.bfloat16)
    blocks = lax.map(one_block, (queries, jnp.arange(SEQUENCE_LENGTH // T_SP, dtype=jnp.int32)))
    return blocks.reshape(SEQUENCE_LENGTH, QH)

def expert_rows(slot_rows, gate_mat, up_mat, down_mat):
    gate_act = jnp.dot(slot_rows, gate_mat, preferred_element_type=jnp.float32)
    up_act = jnp.dot(slot_rows, up_mat, preferred_element_type=jnp.float32)
    hidden = (jax.nn.silu(gate_act) * up_act).astype(jnp.bfloat16)
    return jnp.dot(hidden, down_mat, preferred_element_type=jnp.float32).astype(jnp.bfloat16)

def reference(query_rows, key_rows, value_rows, residual, output_weight, first_gain, first_bias, expert_ids, expert_share, gate_weight, up_weight, down_weight, shared_gate, shared_up, shared_down, second_gain, second_bias):
    attended = stick_attention(query_rows, key_rows, value_rows)
    mixed = jnp.dot(attended, output_weight, preferred_element_type=jnp.float32)
    normed = layer_norm(residual.astype(jnp.float32) + mixed, first_gain, first_bias).astype(jnp.bfloat16)
    sources = SEQUENCE_LENGTH // TOK
    pair_count = TOK * TOP_K
    id_table = expert_ids.reshape(sources, pair_count).astype(jnp.int32)
    one_hot = (id_table[:, :, None] == jnp.arange(EXPERTS, dtype=jnp.int32)[None, None, :]).astype(jnp.int32)
    before = jnp.cumsum(one_hot, axis=1) - one_hot
    ranked = lax.optimization_barrier(jnp.sum(before * one_hot, axis=2)).astype(jnp.int32)
    source_ids = jnp.arange(sources, dtype=jnp.int32)[:, None]
    row_ids = (source_ids * pair_count + jnp.arange(pair_count, dtype=jnp.int32)[None, :]).astype(jnp.int32)
    columns = (source_ids * CAP + ranked).astype(jnp.int32)
    slot_table = jnp.full((EXPERTS, sources * CAP), SEQUENCE_LENGTH * TOP_K, jnp.int32).at[id_table, columns].set(row_ids)
    padded_rows = jnp.concatenate([normed, jnp.zeros((1, D), jnp.bfloat16)], axis=0)
    padded_share = jnp.concatenate([expert_share.reshape(-1).astype(jnp.float32), jnp.zeros((1,), jnp.float32)])

    def per_expert(carry, expert):
        slot_rows = slot_table[expert]
        token_of = (slot_rows // TOP_K).astype(jnp.int32)
        outputs = expert_rows(padded_rows[token_of], gate_weight[expert], up_weight[expert], down_weight[expert])
        shares = padded_share[slot_rows]
        carry = carry.at[token_of].add(outputs.astype(jnp.float32) * shares[:, None])
        return (carry, None)
    routed, _ = lax.scan(per_expert, jnp.zeros((SEQUENCE_LENGTH + 1, D), jnp.float32), jnp.arange(EXPERTS, dtype=jnp.int32))
    routed = routed[:SEQUENCE_LENGTH]
    gate_act = jnp.dot(normed, shared_gate, preferred_element_type=jnp.float32)
    up_act = jnp.dot(normed, shared_up, preferred_element_type=jnp.float32)
    shared_hidden = (jax.nn.silu(gate_act) * up_act).astype(jnp.bfloat16)
    shared_out = jnp.dot(shared_hidden, shared_down, preferred_element_type=jnp.float32)
    final = layer_norm(normed.astype(jnp.float32) + routed + shared_out, second_gain, second_bias)
    return final.astype(jnp.bfloat16)
```

```python
import jax
import jax.numpy as jnp
from jax import lax
from jax.sharding import PartitionSpec as P

HEAD_DIM = 128
KBLK = 128


NORM_EPS = 1e-05


def layer_norm(summed, gains, offset):
    average = jnp.mean(summed, axis=-1, keepdims=True)
    centred = summed - average
    spread = jnp.mean(centred * centred, axis=-1, keepdims=True)
    return centred * lax.rsqrt(spread + NORM_EPS) * gains + offset


def stick_local(query_rows, key_all, value_all, seq_index):
    shard_len = query_rows.shape[0]
    heads_here = query_rows.shape[1] // HEAD_DIM
    step_len = 2 * shard_len
    blocks_per = step_len // KBLK
    scale = HEAD_DIM ** (-0.5)
    queries = query_rows.reshape(shard_len, heads_here, HEAD_DIM)
    query_pos = seq_index * shard_len + jnp.arange(shard_len, dtype=jnp.int32)
    visits = seq_index // 2 + 1
    upper = (jnp.arange(KBLK)[:, None] >= jnp.arange(KBLK)[None, :]).astype(jnp.float32)

    def visit(visit_no, carry):
        summed, behind = carry
        chosen = visits - 1 - visit_no
        first_key = chosen * step_len
        key_block = lax.dynamic_slice_in_dim(key_all, first_key, step_len, 0).reshape(
            step_len, heads_here, HEAD_DIM
        )
        value_block = lax.dynamic_slice_in_dim(value_all, first_key, step_len, 0).reshape(
            blocks_per, KBLK, heads_here, HEAD_DIM
        )
        key_pos = (first_key + jnp.arange(step_len, dtype=jnp.int32)).reshape(blocks_per, KBLK)
        score = (
            jnp.einsum("qhd,khd->qhk", queries, key_block, preferred_element_type=jnp.float32)
            * scale
        )
        score = score.reshape(shard_len, heads_here, blocks_per, KBLK)
        usable = key_pos[None, None, :, :] < query_pos[:, None, None, None]
        spent = jnp.where(usable, jax.nn.softplus(score), 0.0)
        inside = jnp.dot(spent.reshape(-1, KBLK), upper, precision=lax.Precision.HIGHEST).reshape(
            spent.shape
        )
        totals = inside[..., 0]
        weight = jnp.where(usable, jnp.exp(score - inside), 0.0).astype(jnp.bfloat16)
        pieces = jnp.einsum(
            "qhbk,bkhd->qhbd", weight, value_block, preferred_element_type=jnp.float32
        )
        block_running = jnp.cumsum(totals, axis=-1)
        step_total = block_running[..., -1]
        beyond = step_total[..., None] - block_running
        factor = jnp.exp(-(behind[..., None] + beyond))
        summed = summed + jnp.sum(pieces * factor[..., None], axis=2)
        return (summed, behind + step_total)

    initial = (
        jnp.zeros((shard_len, heads_here, HEAD_DIM), jnp.float32),
        jnp.zeros((shard_len, heads_here), jnp.float32),
    )
    summed, _ = lax.fori_loop(0, visits, visit, initial)
    return summed.reshape(shard_len, heads_here * HEAD_DIM).astype(jnp.bfloat16)


def slot_capacity(pair_count, experts):
    return max(2, 3 * pair_count // (2 * experts))


def routed_slots(normed, expert_ids, expert_share, gate_weight, up_weight, down_weight):
    tokens_here, width = normed.shape
    top_count = expert_ids.shape[1]
    pair_count = tokens_here * top_count
    experts = lax.axis_size("sp") * lax.axis_size("tp")
    capacity = slot_capacity(pair_count, experts)
    flat_ids = expert_ids.reshape(pair_count)
    one_hot = (flat_ids[:, None] == jnp.arange(experts, dtype=jnp.int32)[None, :]).astype(
        jnp.bfloat16
    )
    earlier_mask = (jnp.arange(pair_count)[:, None] > jnp.arange(pair_count)[None, :]).astype(
        jnp.bfloat16
    )
    before = jnp.dot(earlier_mask, one_hot, preferred_element_type=jnp.float32)
    ranked = jnp.sum(before * one_hot, axis=1).astype(jnp.int32)
    slot_ids = flat_ids * capacity + ranked
    selector = jnp.any(
        slot_ids.reshape(tokens_here, top_count)[None, :, :]
        == jnp.arange(experts * capacity, dtype=jnp.int32)[:, None, None],
        axis=2,
    )
    outgoing = jnp.dot(selector.astype(jnp.bfloat16), normed, preferred_element_type=jnp.float32)
    outgoing = outgoing.astype(jnp.bfloat16).reshape(experts, capacity, width)
    slot_rows = lax.all_to_all(outgoing, ("sp", "tp"), split_axis=0, concat_axis=0, tiled=True)
    flat_rows = slot_rows.reshape(-1, width)
    gate_act = jnp.dot(flat_rows, gate_weight[0], preferred_element_type=jnp.float32)
    up_act = jnp.dot(flat_rows, up_weight[0], preferred_element_type=jnp.float32)
    hidden = (jax.nn.silu(gate_act) * up_act).astype(jnp.bfloat16)
    produced = jnp.dot(hidden, down_weight[0], preferred_element_type=jnp.float32).astype(
        jnp.bfloat16
    )
    results = produced.reshape(slot_rows.shape)
    returned = lax.all_to_all(results, ("sp", "tp"), split_axis=0, concat_axis=0, tiled=True)
    flat_back = returned.reshape(experts * capacity, width)
    picked = jnp.take(flat_back, slot_ids, axis=0).reshape(tokens_here, top_count, width)
    routed = jnp.sum(picked.astype(jnp.float32) * expert_share[:, :, None], axis=1)
    return routed


def expert_dense(rows, ids_all, share_all, expert, gate_mat, up_mat, down_mat):
    weight = jnp.sum(jnp.where(ids_all == expert, share_all, 0.0), axis=1, keepdims=True)
    gate_act = jnp.dot(rows, gate_mat, preferred_element_type=jnp.float32)
    up_act = jnp.dot(rows, up_mat, preferred_element_type=jnp.float32)
    hidden = (jax.nn.silu(gate_act) * up_act).astype(jnp.bfloat16)
    produced = jnp.dot(hidden, down_mat, preferred_element_type=jnp.float32)
    return (produced * weight).astype(jnp.bfloat16)


def routed_dense(normed, expert_ids, expert_share, gate_weight, up_weight, down_weight):
    axes = ("sp", "tp")
    expert = lax.axis_index("sp") * lax.axis_size("tp") + lax.axis_index("tp")
    rows = lax.all_gather(normed, axes, axis=0, tiled=True)
    ids_all = lax.all_gather(expert_ids, axes, axis=0, tiled=True)
    share_all = lax.all_gather(expert_share, axes, axis=0, tiled=True)
    parts = expert_dense(
        rows, ids_all, share_all, expert, gate_weight[0], up_weight[0], down_weight[0]
    )
    return lax.psum_scatter(parts, axes, scatter_dimension=0, tiled=True).astype(jnp.float32)


def local(
    query_rows,
    key_rows,
    value_rows,
    residual,
    output_weight,
    first_gain,
    first_bias,
    expert_ids,
    expert_share,
    gate_weight,
    up_weight,
    down_weight,
    shared_gate,
    shared_up,
    shared_down,
    second_gain,
    second_bias,
):
    seq_index = lax.axis_index("sp")
    key_all, value_all = (
        lax.all_gather(key_rows, "sp", axis=0, tiled=True),
        lax.all_gather(value_rows, "sp", axis=0, tiled=True),
    )
    attended = stick_local(query_rows, key_all, value_all, seq_index)
    tokens_here = residual.shape[0]
    by_token = lax.all_to_all(attended, "tp", split_axis=0, concat_axis=1, tiled=True)
    mixed = jnp.dot(
        by_token,
        lax.all_gather(output_weight, "tp", axis=0, tiled=True),
        preferred_element_type=jnp.float32,
    )
    normed = layer_norm(residual.astype(jnp.float32) + mixed, first_gain, first_bias).astype(
        jnp.bfloat16
    )
    experts = lax.axis_size("sp") * lax.axis_size("tp")
    slots = experts * slot_capacity(tokens_here * expert_ids.shape[1], experts)
    routed_fn = routed_dense if tokens_here * experts <= 4 * slots else routed_slots
    routed = routed_fn(normed, expert_ids, expert_share, gate_weight, up_weight, down_weight)
    gate_act = jnp.dot(normed, shared_gate, preferred_element_type=jnp.float32)
    up_act = jnp.dot(normed, shared_up, preferred_element_type=jnp.float32)
    shared_hidden = (jax.nn.silu(gate_act) * up_act).astype(jnp.bfloat16)
    shared_out = jnp.dot(shared_hidden, shared_down, preferred_element_type=jnp.float32)
    final = layer_norm(normed.astype(jnp.float32) + routed + shared_out, second_gain, second_bias)
    return final.astype(jnp.bfloat16)


def solution(mesh):
    return jax.shard_map(
        local,
        mesh=mesh,
        in_specs=(
            P(("grp", "sp"), "tp"),
            P(("grp", "sp"), "tp"),
            P(("grp", "sp"), "tp"),
            P(("grp", "sp", "tp"), None),
            P("tp", None),
            P(),
            P(),
            P(("grp", "sp", "tp"), None),
            P(("grp", "sp", "tp"), None),
            P(("sp", "tp"), None, None),
            P(("sp", "tp"), None, None),
            P(("sp", "tp"), None, None),
            P(),
            P(),
            P(),
            P(),
            P(),
        ),
        out_specs=P(("grp", "sp", "tp"), None),
        check_vma=False,
    )
```

```python
import functools

import jax
import jax.numpy as jnp
from jax import lax
from jax.experimental import pallas as pl
from jax.experimental.pallas import tpu as pltpu
from jax.sharding import PartitionSpec as P

HEAD_DIM = 128
KBLK = 128


NORM_EPS = 1e-05


def layer_norm(summed, gains, offset):
    average = jnp.mean(summed, axis=-1, keepdims=True)
    centred = summed - average
    spread = jnp.mean(centred * centred, axis=-1, keepdims=True)
    return centred * lax.rsqrt(spread + NORM_EPS) * gains + offset


def stick_local(query_rows, key_all, value_all, seq_index):
    shard_len = query_rows.shape[0]
    heads_here = query_rows.shape[1] // HEAD_DIM
    step_len = 2 * shard_len
    blocks_per = step_len // KBLK
    scale = HEAD_DIM ** (-0.5)
    queries = query_rows.reshape(shard_len, heads_here, HEAD_DIM)
    query_pos = seq_index * shard_len + jnp.arange(shard_len, dtype=jnp.int32)
    visits = seq_index // 2 + 1
    upper = (jnp.arange(KBLK)[:, None] >= jnp.arange(KBLK)[None, :]).astype(jnp.float32)

    def visit(visit_no, carry):
        summed, behind = carry
        chosen = visits - 1 - visit_no
        first_key = chosen * step_len
        key_block = lax.dynamic_slice_in_dim(key_all, first_key, step_len, 0).reshape(
            step_len, heads_here, HEAD_DIM
        )
        value_block = lax.dynamic_slice_in_dim(value_all, first_key, step_len, 0).reshape(
            blocks_per, KBLK, heads_here, HEAD_DIM
        )
        key_pos = (first_key + jnp.arange(step_len, dtype=jnp.int32)).reshape(blocks_per, KBLK)
        score = (
            jnp.einsum("qhd,khd->qhk", queries, key_block, preferred_element_type=jnp.float32)
            * scale
        )
        score = score.reshape(shard_len, heads_here, blocks_per, KBLK)
        usable = key_pos[None, None, :, :] < query_pos[:, None, None, None]
        spent = jnp.where(usable, jax.nn.softplus(score), 0.0)
        inside = jnp.dot(spent.reshape(-1, KBLK), upper, precision=lax.Precision.HIGHEST).reshape(
            spent.shape
        )
        totals = inside[..., 0]
        weight = jnp.where(usable, jnp.exp(score - inside), 0.0).astype(jnp.bfloat16)
        pieces = jnp.einsum(
            "qhbk,bkhd->qhbd", weight, value_block, preferred_element_type=jnp.float32
        )
        block_running = jnp.cumsum(totals, axis=-1)
        step_total = block_running[..., -1]
        beyond = step_total[..., None] - block_running
        factor = jnp.exp(-(behind[..., None] + beyond))
        summed = summed + jnp.sum(pieces * factor[..., None], axis=2)
        return (summed, behind + step_total)

    initial = (
        jnp.zeros((shard_len, heads_here, HEAD_DIM), jnp.float32),
        jnp.zeros((shard_len, heads_here), jnp.float32),
    )
    summed, _ = lax.fori_loop(0, visits, visit, initial)
    return summed.reshape(shard_len, heads_here * HEAD_DIM).astype(jnp.bfloat16)


def exchange_kernel(n_sp, n_tp, src, dst, send_sem, recv_sem, own_sem):
    count = n_sp * n_tp
    me = lax.axis_index("sp") * n_tp + lax.axis_index("tp")

    def place(peer):
        return {"sp": peer // n_tp, "tp": lax.rem(peer, n_tp)}

    def copy(step, peer, landing):
        return pltpu.make_async_remote_copy(
            src_ref=src.at[peer],
            dst_ref=dst.at[landing],
            send_sem=send_sem.at[step],
            recv_sem=recv_sem.at[step],
            device_id=place(peer),
            device_id_type=pl.DeviceIdType.MESH,
        )

    barrier = pltpu.get_barrier_semaphore()

    @pl.loop(1, count)
    def _(step):
        peer = lax.rem(me + step, count)
        pl.semaphore_signal(
            barrier, inc=1, device_id=place(peer), device_id_type=pl.DeviceIdType.MESH
        )

    pl.semaphore_wait(barrier, count - 1)
    own = pltpu.make_async_copy(src.at[me], dst.at[me], own_sem)
    own.start()

    @pl.loop(1, count)
    def _(step):
        copy(step, lax.rem(me + step, count), me).start()

    own.wait()

    @pl.loop(1, count)
    def _(step):
        copy(step, lax.rem(me + step, count), lax.rem(me + count - step, count)).wait()


def exchange(blocks, collective_id):
    n_sp, n_tp = lax.axis_size("sp"), lax.axis_size("tp")
    return pl.pallas_call(
        functools.partial(exchange_kernel, n_sp, n_tp),
        out_shape=jax.ShapeDtypeStruct(blocks.shape, blocks.dtype),
        in_specs=[pl.BlockSpec(memory_space=pl.ANY)],
        out_specs=pl.BlockSpec(memory_space=pl.ANY),
        scratch_shapes=[
            pltpu.SemaphoreType.DMA((n_sp * n_tp,)),
            pltpu.SemaphoreType.DMA((n_sp * n_tp,)),
            pltpu.SemaphoreType.DMA,
        ],
        compiler_params=pltpu.CompilerParams(
            collective_id=collective_id, has_side_effects=True
        ),
    )(blocks)


def local(
    query_rows,
    key_rows,
    value_rows,
    residual,
    output_weight,
    first_gain,
    first_bias,
    expert_ids,
    expert_share,
    gate_weight,
    up_weight,
    down_weight,
    shared_gate,
    shared_up,
    shared_down,
    second_gain,
    second_bias,
):
    seq_index = lax.axis_index("sp")
    key_all, value_all = (
        lax.all_gather(key_rows, "sp", axis=0, tiled=True),
        lax.all_gather(value_rows, "sp", axis=0, tiled=True),
    )
    attended = stick_local(query_rows, key_all, value_all, seq_index)
    tokens_here = residual.shape[0]
    width = residual.shape[1]
    by_token = lax.all_to_all(attended, "tp", split_axis=0, concat_axis=1, tiled=True)
    mixed = jnp.dot(
        by_token,
        lax.all_gather(output_weight, "tp", axis=0, tiled=True),
        preferred_element_type=jnp.float32,
    )
    normed = layer_norm(residual.astype(jnp.float32) + mixed, first_gain, first_bias).astype(
        jnp.bfloat16
    )
    top_count = expert_ids.shape[1]
    pair_count = tokens_here * top_count
    experts = lax.axis_size("sp") * lax.axis_size("tp")
    capacity = max(2, 3 * pair_count // (2 * experts))
    flat_ids = expert_ids.reshape(pair_count)
    one_hot = (flat_ids[:, None] == jnp.arange(experts, dtype=jnp.int32)[None, :]).astype(
        jnp.bfloat16
    )
    earlier_mask = (jnp.arange(pair_count)[:, None] > jnp.arange(pair_count)[None, :]).astype(
        jnp.bfloat16
    )
    before = jnp.dot(earlier_mask, one_hot, preferred_element_type=jnp.float32)
    ranked = jnp.sum(before * one_hot, axis=1).astype(jnp.int32)
    slot_ids = flat_ids * capacity + ranked
    selector = jnp.any(
        slot_ids.reshape(tokens_here, top_count)[None, :, :]
        == jnp.arange(experts * capacity, dtype=jnp.int32)[:, None, None],
        axis=2,
    )
    outgoing = jnp.dot(selector.astype(jnp.bfloat16), normed, preferred_element_type=jnp.float32)
    outgoing = outgoing.astype(jnp.bfloat16).reshape(experts, capacity, width)
    slot_rows = exchange(outgoing, 1)
    flat_rows = slot_rows.reshape(-1, width)
    gate_act = jnp.dot(flat_rows, gate_weight[0], preferred_element_type=jnp.float32)
    up_act = jnp.dot(flat_rows, up_weight[0], preferred_element_type=jnp.float32)
    hidden = (jax.nn.silu(gate_act) * up_act).astype(jnp.bfloat16)
    produced = jnp.dot(hidden, down_weight[0], preferred_element_type=jnp.float32).astype(
        jnp.bfloat16
    )
    results = produced.reshape(slot_rows.shape)
    returned = exchange(results, 2)
    flat_back = returned.reshape(experts * capacity, width)
    placed = slot_ids.reshape(tokens_here, top_count)[:, :, None] == jnp.arange(
        experts * capacity, dtype=jnp.int32
    )
    shares = jnp.sum(jnp.where(placed, expert_share[:, :, None], 0.0), axis=1)
    upper_part = lax.reduce_precision(shares, 8, 7)
    both = jnp.concatenate([upper_part, shares - upper_part], axis=0).astype(jnp.bfloat16)
    both_out = jnp.dot(both, flat_back, preferred_element_type=jnp.float32)
    routed = both_out[:tokens_here] + both_out[tokens_here:]
    gate_act = jnp.dot(normed, shared_gate, preferred_element_type=jnp.float32)
    up_act = jnp.dot(normed, shared_up, preferred_element_type=jnp.float32)
    shared_hidden = (jax.nn.silu(gate_act) * up_act).astype(jnp.bfloat16)
    shared_out = jnp.dot(shared_hidden, shared_down, preferred_element_type=jnp.float32)
    final = layer_norm(normed.astype(jnp.float32) + routed + shared_out, second_gain, second_bias)
    return final.astype(jnp.bfloat16)


def solution(mesh):
    return jax.shard_map(
        local,
        mesh=mesh,
        in_specs=(
            P(("grp", "sp"), "tp"),
            P(("grp", "sp"), "tp"),
            P(("grp", "sp"), "tp"),
            P(("grp", "sp", "tp"), None),
            P("tp", None),
            P(),
            P(),
            P(("grp", "sp", "tp"), None),
            P(("grp", "sp", "tp"), None),
            P(("sp", "tp"), None, None),
            P(("sp", "tp"), None, None),
            P(("sp", "tp"), None, None),
            P(),
            P(),
            P(),
            P(),
            P(),
        ),
        out_specs=P(("grp", "sp", "tp"), None),
        check_vma=False,
    )
```

```python
import functools

import jax
import jax.numpy as jnp
from jax import lax
from jax.experimental import pallas as pl
from jax.experimental.pallas import tpu as pltpu
from jax.sharding import PartitionSpec as P

HEAD_DIM = 128
KBLK = 128


NORM_EPS = 1e-05


def layer_norm(summed, gains, offset):
    average = jnp.mean(summed, axis=-1, keepdims=True)
    centred = summed - average
    spread = jnp.mean(centred * centred, axis=-1, keepdims=True)
    return centred * lax.rsqrt(spread + NORM_EPS) * gains + offset


def three_parts(exact):
    high = exact.astype(jnp.bfloat16)
    rest = exact - high.astype(jnp.float32)
    middle = rest.astype(jnp.bfloat16)
    low = (rest - middle.astype(jnp.float32)).astype(jnp.bfloat16)
    return jnp.concatenate([high, middle, low], axis=1)


def mixer_kernel(
    n_sp,
    n_tp,
    query_ref,
    key_ref,
    value_ref,
    weight_ref,
    parts_ref,
    weights_ref,
    held,
    summed,
    behind,
    ready,
    held_send,
    held_recv,
    weight_send,
    weight_recv,
    part_send,
    part_recv,
    own_sem,
):
    mesh_ids = pl.DeviceIdType.MESH
    seq_index, tp_index = lax.axis_index("sp"), lax.axis_index("tp")
    shard_len, features = query_ref.shape
    tokens = shard_len // n_tp
    heads = features // HEAD_DIM
    tile = min(shard_len, 256)
    scale = HEAD_DIM ** (-0.5)
    has_next, has_last = seq_index < n_sp - 1, seq_index > 0
    after, ahead = lax.rem(seq_index + 1, n_sp), lax.rem(seq_index + n_sp - 1, n_sp)

    barrier = pltpu.get_barrier_semaphore()

    @pl.when(has_next)
    def _():
        pl.semaphore_signal(barrier, inc=1, device_id={"sp": after}, device_id_type=mesh_ids)

    @pl.when(has_last)
    def _():
        pl.semaphore_signal(barrier, inc=1, device_id={"sp": ahead}, device_id_type=mesh_ids)

    for step in range(1, n_tp):
        peer = lax.rem(tp_index + step, n_tp)
        pl.semaphore_signal(barrier, inc=1, device_id={"tp": peer}, device_id_type=mesh_ids)

    own_copies = [
        pltpu.make_async_copy(key_ref, held.at[seq_index, 0], own_sem.at[0]),
        pltpu.make_async_copy(value_ref, held.at[seq_index, 1], own_sem.at[1]),
        pltpu.make_async_copy(weight_ref, weights_ref.at[tp_index], own_sem.at[2]),
    ]
    for copy in own_copies:
        copy.start()
    summed[...] = jnp.zeros_like(summed)
    behind[...] = jnp.zeros_like(behind)
    pl.semaphore_wait(
        barrier, n_tp - 1 + has_next.astype(jnp.int32) + has_last.astype(jnp.int32)
    )

    def held_copy(step, which):
        block = lax.rem(seq_index - step + n_sp, n_sp)
        return pltpu.make_async_remote_copy(
            src_ref=held.at[block, which],
            dst_ref=held.at[block, which],
            send_sem=held_send.at[step, which],
            recv_sem=held_recv.at[step, which],
            device_id={"sp": after},
            device_id_type=mesh_ids,
        )

    def arrived(step, which):
        block = lax.rem(seq_index - step + n_sp, n_sp)
        return pltpu.make_async_remote_copy(
            src_ref=held.at[block, which],
            dst_ref=held.at[block, which],
            send_sem=held_send.at[step - 1, which],
            recv_sem=held_recv.at[step - 1, which],
            device_id={"sp": after},
            device_id_type=mesh_ids,
        )

    def weight_copy(step, landing):
        return pltpu.make_async_remote_copy(
            src_ref=weight_ref,
            dst_ref=weights_ref.at[landing],
            send_sem=weight_send.at[step],
            recv_sem=weight_recv.at[step],
            device_id={"tp": lax.rem(tp_index + step, n_tp)},
            device_id_type=mesh_ids,
        )

    def part_copy(step, landing):
        peer = lax.rem(tp_index + step, n_tp)
        return pltpu.make_async_remote_copy(
            src_ref=ready.at[peer],
            dst_ref=parts_ref.at[landing],
            send_sem=part_send.at[step],
            recv_sem=part_recv.at[step],
            device_id={"tp": peer},
            device_id_type=mesh_ids,
        )

    for copy in own_copies:
        copy.wait()

    @pl.when(has_next)
    def _():
        for which in range(2):
            held_copy(0, which).start()

    for step in range(1, n_tp):
        weight_copy(step, tp_index).start()

    key_lane = lax.broadcasted_iota(jnp.int32, (tile, KBLK), 1)
    query_row = lax.broadcasted_iota(jnp.int32, (tile, KBLK), 0)
    from_row = lax.broadcasted_iota(jnp.int32, (KBLK, 2 * KBLK), 0)
    to_lane = lax.broadcasted_iota(jnp.int32, (KBLK, 2 * KBLK), 1)
    reach = ((from_row >= to_lane) | (to_lane >= KBLK)).astype(jnp.float32).astype(jnp.bfloat16)
    reach = jnp.concatenate([reach, reach, reach], axis=0)

    @pl.loop(0, seq_index + 1)
    def _(step):
        @pl.when(step > 0)
        def _():
            for which in range(2):
                arrived(step, which).wait_recv()

            @pl.when(has_next)
            def _():
                for which in range(2):
                    held_copy(step, which).start()

        block = seq_index - step
        for head in range(heads):
            lanes = slice(head * HEAD_DIM, (head + 1) * HEAD_DIM)
            for first_key in reversed(range(0, shard_len, KBLK)):
                key_block = held[block, 0, first_key : first_key + KBLK, lanes]
                value_block = held[block, 1, first_key : first_key + KBLK, lanes]
                for first_query in range(0, shard_len, tile):
                    rows = slice(first_query, first_query + tile)
                    score = scale * lax.dot_general(
                        query_ref[rows, lanes],
                        key_block,
                        (((1,), (1,)), ((), ())),
                        preferred_element_type=jnp.float32,
                    )
                    usable = (key_lane + first_key) < (
                        query_row + (first_query + step * shard_len)
                    )
                    grown = jnp.maximum(score, 0.0) + jnp.log(1.0 + jnp.exp(-jnp.abs(score)))
                    spent = jnp.where(usable, grown, 0.0)
                    sums = jnp.dot(three_parts(spent), reach, preferred_element_type=jnp.float32)
                    share = jnp.where(usable, jnp.exp(score - sums[:, :KBLK]), 0.0)
                    piece = jnp.dot(
                        share.astype(jnp.bfloat16),
                        value_block,
                        preferred_element_type=jnp.float32,
                    )
                    before = behind[head, rows, :]
                    summed[rows, lanes] += piece * jnp.exp(-before)
                    behind[head, rows, :] = before + sums[:, KBLK:]

    for peer in range(n_tp):
        ready[peer] = summed[peer * tokens : (peer + 1) * tokens, :].astype(jnp.bfloat16)
    for step in range(1, n_tp):
        part_copy(step, tp_index).start()
    parts_ref[tp_index] = ready[tp_index]

    @pl.when(has_next)
    def _():
        @pl.loop(0, seq_index + 1)
        def _(step):
            for which in range(2):
                held_copy(step, which).wait_send()

    for step in range(1, n_tp):
        source = lax.rem(tp_index + n_tp - step, n_tp)
        weight_copy(step, source).wait()
        part_copy(step, source).wait()


def mixer(query_rows, key_rows, value_rows, output_weight):
    n_sp, n_tp = lax.axis_size("sp"), lax.axis_size("tp")
    shard_len, features = query_rows.shape
    tokens = shard_len // n_tp
    heads = features // HEAD_DIM
    in_vmem = pl.BlockSpec(memory_space=pltpu.VMEM)
    dma = pltpu.SemaphoreType.DMA
    parts, weights = pl.pallas_call(
        functools.partial(mixer_kernel, n_sp, n_tp),
        out_shape=(
            jax.ShapeDtypeStruct((n_tp, tokens, features), jnp.bfloat16),
            jax.ShapeDtypeStruct((n_tp,) + output_weight.shape, output_weight.dtype),
        ),
        in_specs=[in_vmem] * 4,
        out_specs=(in_vmem, in_vmem),
        scratch_shapes=[
            pltpu.VMEM((n_sp, 2, shard_len, features), jnp.bfloat16),
            pltpu.VMEM((shard_len, features), jnp.float32),
            pltpu.VMEM((heads, shard_len, KBLK), jnp.float32),
            pltpu.VMEM((n_tp, tokens, features), jnp.bfloat16),
            dma((n_sp, 2)),
            dma((n_sp, 2)),
            dma((n_tp,)),
            dma((n_tp,)),
            dma((n_tp,)),
            dma((n_tp,)),
            dma((3,)),
        ],
        compiler_params=pltpu.CompilerParams(collective_id=3, has_side_effects=True),
    )(query_rows, key_rows, value_rows, output_weight)
    by_token = jnp.concatenate([parts[index] for index in range(n_tp)], axis=1)
    return by_token, weights.reshape(-1, output_weight.shape[1])


def exchange_kernel(n_sp, n_tp, src, dst, send_sem, recv_sem, own_sem):
    count = n_sp * n_tp
    me = lax.axis_index("sp") * n_tp + lax.axis_index("tp")

    def place(peer):
        return {"sp": peer // n_tp, "tp": lax.rem(peer, n_tp)}

    def copy(step, peer, landing):
        return pltpu.make_async_remote_copy(
            src_ref=src.at[peer],
            dst_ref=dst.at[landing],
            send_sem=send_sem.at[step],
            recv_sem=recv_sem.at[step],
            device_id=place(peer),
            device_id_type=pl.DeviceIdType.MESH,
        )

    barrier = pltpu.get_barrier_semaphore()

    @pl.loop(1, count)
    def _(step):
        peer = lax.rem(me + step, count)
        pl.semaphore_signal(
            barrier, inc=1, device_id=place(peer), device_id_type=pl.DeviceIdType.MESH
        )

    pl.semaphore_wait(barrier, count - 1)
    own = pltpu.make_async_copy(src.at[me], dst.at[me], own_sem)
    own.start()

    @pl.loop(1, count)
    def _(step):
        copy(step, lax.rem(me + step, count), me).start()

    own.wait()

    @pl.loop(1, count)
    def _(step):
        copy(step, lax.rem(me + step, count), lax.rem(me + count - step, count)).wait()


def exchange(blocks, collective_id):
    n_sp, n_tp = lax.axis_size("sp"), lax.axis_size("tp")
    return pl.pallas_call(
        functools.partial(exchange_kernel, n_sp, n_tp),
        out_shape=jax.ShapeDtypeStruct(blocks.shape, blocks.dtype),
        in_specs=[pl.BlockSpec(memory_space=pl.ANY)],
        out_specs=pl.BlockSpec(memory_space=pl.ANY),
        scratch_shapes=[
            pltpu.SemaphoreType.DMA((n_sp * n_tp,)),
            pltpu.SemaphoreType.DMA((n_sp * n_tp,)),
            pltpu.SemaphoreType.DMA,
        ],
        compiler_params=pltpu.CompilerParams(
            collective_id=collective_id, has_side_effects=True
        ),
    )(blocks)


def local(
    query_rows,
    key_rows,
    value_rows,
    residual,
    output_weight,
    first_gain,
    first_bias,
    expert_ids,
    expert_share,
    gate_weight,
    up_weight,
    down_weight,
    shared_gate,
    shared_up,
    shared_down,
    second_gain,
    second_bias,
):
    by_token, weights = mixer(query_rows, key_rows, value_rows, output_weight)
    tokens_here = residual.shape[0]
    width = residual.shape[1]
    mixed = jnp.dot(by_token, weights, preferred_element_type=jnp.float32)
    normed = layer_norm(residual.astype(jnp.float32) + mixed, first_gain, first_bias).astype(
        jnp.bfloat16
    )
    top_count = expert_ids.shape[1]
    pair_count = tokens_here * top_count
    experts = lax.axis_size("sp") * lax.axis_size("tp")
    capacity = max(2, 3 * pair_count // (2 * experts))
    flat_ids = expert_ids.reshape(pair_count)
    one_hot = (flat_ids[:, None] == jnp.arange(experts, dtype=jnp.int32)[None, :]).astype(
        jnp.bfloat16
    )
    earlier_mask = (jnp.arange(pair_count)[:, None] > jnp.arange(pair_count)[None, :]).astype(
        jnp.bfloat16
    )
    before = jnp.dot(earlier_mask, one_hot, preferred_element_type=jnp.float32)
    ranked = jnp.sum(before * one_hot, axis=1).astype(jnp.int32)
    slot_ids = flat_ids * capacity + ranked
    selector = jnp.any(
        slot_ids.reshape(tokens_here, top_count)[None, :, :]
        == jnp.arange(experts * capacity, dtype=jnp.int32)[:, None, None],
        axis=2,
    )
    outgoing = jnp.dot(selector.astype(jnp.bfloat16), normed, preferred_element_type=jnp.float32)
    outgoing = outgoing.astype(jnp.bfloat16).reshape(experts, capacity, width)
    slot_rows = exchange(outgoing, 1)
    flat_rows = slot_rows.reshape(-1, width)
    gate_act = jnp.dot(flat_rows, gate_weight[0], preferred_element_type=jnp.float32)
    up_act = jnp.dot(flat_rows, up_weight[0], preferred_element_type=jnp.float32)
    hidden = (jax.nn.silu(gate_act) * up_act).astype(jnp.bfloat16)
    produced = jnp.dot(hidden, down_weight[0], preferred_element_type=jnp.float32).astype(
        jnp.bfloat16
    )
    results = produced.reshape(slot_rows.shape)
    returned = lax.all_to_all(results, ("sp", "tp"), split_axis=0, concat_axis=0, tiled=True)
    flat_back = returned.reshape(experts * capacity, width)
    placed = slot_ids.reshape(tokens_here, top_count)[:, :, None] == jnp.arange(
        experts * capacity, dtype=jnp.int32
    )
    shares = jnp.sum(jnp.where(placed, expert_share[:, :, None], 0.0), axis=1)
    upper_part = lax.reduce_precision(shares, 8, 7)
    both = jnp.concatenate([upper_part, shares - upper_part], axis=0).astype(jnp.bfloat16)
    both_out = jnp.dot(both, flat_back, preferred_element_type=jnp.float32)
    routed = both_out[:tokens_here] + both_out[tokens_here:]
    gate_act = jnp.dot(normed, shared_gate, preferred_element_type=jnp.float32)
    up_act = jnp.dot(normed, shared_up, preferred_element_type=jnp.float32)
    shared_hidden = (jax.nn.silu(gate_act) * up_act).astype(jnp.bfloat16)
    shared_out = jnp.dot(shared_hidden, shared_down, preferred_element_type=jnp.float32)
    final = layer_norm(normed.astype(jnp.float32) + routed + shared_out, second_gain, second_bias)
    return final.astype(jnp.bfloat16)


def solution(mesh):
    return jax.shard_map(
        local,
        mesh=mesh,
        in_specs=(
            P(("grp", "sp"), "tp"),
            P(("grp", "sp"), "tp"),
            P(("grp", "sp"), "tp"),
            P(("grp", "sp", "tp"), None),
            P("tp", None),
            P(),
            P(),
            P(("grp", "sp", "tp"), None),
            P(("grp", "sp", "tp"), None),
            P(("sp", "tp"), None, None),
            P(("sp", "tp"), None, None),
            P(("sp", "tp"), None, None),
            P(),
            P(),
            P(),
            P(),
            P(),
        ),
        out_specs=P(("grp", "sp", "tp"), None),
        check_vma=False,
    )
```

```python
import functools

import jax
import jax.numpy as jnp
from jax import lax
from jax.experimental import pallas as pl
from jax.experimental.pallas import tpu as pltpu
from jax.sharding import PartitionSpec as P

HEAD_DIM = 128
KBLK = 128


NORM_EPS = 1e-05


def layer_norm(summed, gains, offset):
    average = jnp.mean(summed, axis=-1, keepdims=True)
    centred = summed - average
    spread = jnp.mean(centred * centred, axis=-1, keepdims=True)
    return centred * lax.rsqrt(spread + NORM_EPS) * gains + offset


def three_parts(exact):
    high = exact.astype(jnp.bfloat16)
    rest = exact - high.astype(jnp.float32)
    middle = rest.astype(jnp.bfloat16)
    low = (rest - middle.astype(jnp.float32)).astype(jnp.bfloat16)
    return jnp.concatenate([high, middle, low], axis=1)


def mixer_kernel(
    n_sp,
    n_tp,
    query_ref,
    key_ref,
    value_ref,
    weight_ref,
    parts_ref,
    weights_ref,
    held,
    summed,
    behind,
    ready,
    held_send,
    held_recv,
    weight_send,
    weight_recv,
    part_send,
    part_recv,
    pass_send,
    pass_recv,
    own_sem,
):
    mesh_ids = pl.DeviceIdType.MESH
    seq_index, tp_index = lax.axis_index("sp"), lax.axis_index("tp")
    shard_len, features = query_ref.shape
    tokens = shard_len // n_tp
    heads = features // HEAD_DIM
    tile = min(shard_len, 256)
    scale = HEAD_DIM ** (-0.5)
    has_next, has_last = seq_index < n_sp - 1, seq_index > 0
    after, ahead = lax.rem(seq_index + 1, n_sp), lax.rem(seq_index + n_sp - 1, n_sp)

    barrier = pltpu.get_barrier_semaphore()

    @pl.when(has_next)
    def _():
        pl.semaphore_signal(barrier, inc=1, device_id={"sp": after}, device_id_type=mesh_ids)

    @pl.when(has_last)
    def _():
        pl.semaphore_signal(barrier, inc=1, device_id={"sp": ahead}, device_id_type=mesh_ids)

    for step in range(1, n_tp):
        peer = lax.rem(tp_index + step, n_tp)
        pl.semaphore_signal(barrier, inc=1, device_id={"tp": peer}, device_id_type=mesh_ids)

    own_copies = [
        pltpu.make_async_copy(key_ref, held.at[seq_index, 0], own_sem.at[0]),
        pltpu.make_async_copy(value_ref, held.at[seq_index, 1], own_sem.at[1]),
        pltpu.make_async_copy(weight_ref, weights_ref.at[tp_index], own_sem.at[2]),
    ]
    for copy in own_copies:
        copy.start()
    summed[...] = jnp.zeros_like(summed)
    behind[...] = jnp.zeros_like(behind)
    pl.semaphore_wait(
        barrier, n_tp - 1 + has_next.astype(jnp.int32) + has_last.astype(jnp.int32)
    )

    def held_copy(step, which):
        block = lax.rem(seq_index - step + n_sp, n_sp)
        return pltpu.make_async_remote_copy(
            src_ref=held.at[block, which],
            dst_ref=held.at[block, which],
            send_sem=held_send.at[step, which],
            recv_sem=held_recv.at[step, which],
            device_id={"sp": after},
            device_id_type=mesh_ids,
        )

    def arrived(step, which):
        block = lax.rem(seq_index - step + n_sp, n_sp)
        return pltpu.make_async_remote_copy(
            src_ref=held.at[block, which],
            dst_ref=held.at[block, which],
            send_sem=held_send.at[step - 1, which],
            recv_sem=held_recv.at[step - 1, which],
            device_id={"sp": after},
            device_id_type=mesh_ids,
        )

    pair, side = tp_index // 2, lax.rem(tp_index, 2)
    pairs = n_tp // 2
    half = weight_ref.shape[0] // 2
    sibling = tp_index + 1 - 2 * side

    def sibling_copy(landing):
        return pltpu.make_async_remote_copy(
            src_ref=weight_ref,
            dst_ref=weights_ref.at[landing],
            send_sem=weight_send.at[0],
            recv_sem=weight_recv.at[0],
            device_id={"tp": sibling},
            device_id_type=mesh_ids,
        )

    def half_rows(which):
        return pl.ds(pl.multiple_of(which * half, half), half)

    def slot(step, which):
        return 1 + (step - 1) * 2 + which

    def half_send(step, which):
        target = lax.rem(pair + step, pairs) * 2 + which
        return pltpu.make_async_remote_copy(
            src_ref=weight_ref.at[half_rows(which)],
            dst_ref=weights_ref.at[tp_index, half_rows(which)],
            send_sem=weight_send.at[slot(step, which)],
            recv_sem=weight_recv.at[slot(step, side)],
            device_id={"tp": target},
            device_id_type=mesh_ids,
        )

    def half_arrived(step, which):
        source = lax.rem(pair + pairs - step, pairs) * 2 + which
        place = weights_ref.at[source, half_rows(side)]
        return pltpu.make_async_remote_copy(
            src_ref=place,
            dst_ref=place,
            send_sem=weight_send.at[slot(step, which)],
            recv_sem=weight_recv.at[slot(step, which)],
            device_id={"tp": source},
            device_id_type=mesh_ids,
        )

    def half_pass(step, which, part):
        source = lax.rem(pair + pairs - step, pairs) * 2 + which
        place = weights_ref.at[source, half_rows(part)]
        return pltpu.make_async_remote_copy(
            src_ref=place,
            dst_ref=place,
            send_sem=pass_send.at[slot(step, which)],
            recv_sem=pass_recv.at[slot(step, which)],
            device_id={"tp": sibling},
            device_id_type=mesh_ids,
        )

    others = [(step, which) for step in range(1, pairs) for which in range(2)]

    def part_copy(step, landing):
        peer = lax.rem(tp_index + step, n_tp)
        return pltpu.make_async_remote_copy(
            src_ref=ready.at[peer],
            dst_ref=parts_ref.at[landing],
            send_sem=part_send.at[step],
            recv_sem=part_recv.at[step],
            device_id={"tp": peer},
            device_id_type=mesh_ids,
        )

    for copy in own_copies:
        copy.wait()

    @pl.when(has_next)
    def _():
        for which in range(2):
            held_copy(0, which).start()

    for step, which in others:
        half_send(step, which).start()
    sibling_copy(tp_index).start()

    key_lane = lax.broadcasted_iota(jnp.int32, (tile, KBLK), 1)
    query_row = lax.broadcasted_iota(jnp.int32, (tile, KBLK), 0)
    from_row = lax.broadcasted_iota(jnp.int32, (KBLK, 2 * KBLK), 0)
    to_lane = lax.broadcasted_iota(jnp.int32, (KBLK, 2 * KBLK), 1)
    reach = ((from_row >= to_lane) | (to_lane >= KBLK)).astype(jnp.float32).astype(jnp.bfloat16)
    reach = jnp.concatenate([reach, reach, reach], axis=0)

    @pl.loop(0, seq_index + 1)
    def _(step):
        @pl.when(step > 0)
        def _():
            for which in range(2):
                arrived(step, which).wait_recv()

            @pl.when(has_next)
            def _():
                for which in range(2):
                    held_copy(step, which).start()

        block = seq_index - step
        for head in range(heads):
            lanes = slice(head * HEAD_DIM, (head + 1) * HEAD_DIM)
            for first_key in reversed(range(0, shard_len, KBLK)):
                key_block = held[block, 0, first_key : first_key + KBLK, lanes]
                value_block = held[block, 1, first_key : first_key + KBLK, lanes]
                for first_query in range(0, shard_len, tile):
                    rows = slice(first_query, first_query + tile)
                    score = scale * lax.dot_general(
                        query_ref[rows, lanes],
                        key_block,
                        (((1,), (1,)), ((), ())),
                        preferred_element_type=jnp.float32,
                    )
                    usable = (key_lane + first_key) < (
                        query_row + (first_query + step * shard_len)
                    )
                    grown = jnp.maximum(score, 0.0) + jnp.log(1.0 + jnp.exp(-jnp.abs(score)))
                    spent = jnp.where(usable, grown, 0.0)
                    sums = jnp.dot(three_parts(spent), reach, preferred_element_type=jnp.float32)
                    share = jnp.where(usable, jnp.exp(score - sums[:, :KBLK]), 0.0)
                    piece = jnp.dot(
                        share.astype(jnp.bfloat16),
                        value_block,
                        preferred_element_type=jnp.float32,
                    )
                    before = behind[head, rows, :]
                    summed[rows, lanes] += piece * jnp.exp(-before)
                    behind[head, rows, :] = before + sums[:, KBLK:]

    for peer in range(n_tp):
        ready[peer] = summed[peer * tokens : (peer + 1) * tokens, :].astype(jnp.bfloat16)
    for step in range(1, n_tp):
        part_copy(step, tp_index).start()
    parts_ref[tp_index] = ready[tp_index]
    for step, which in others:
        half_arrived(step, which).wait_recv()
        half_pass(step, which, side).start()

    @pl.when(has_next)
    def _():
        @pl.loop(0, seq_index + 1)
        def _(step):
            for which in range(2):
                held_copy(step, which).wait_send()

    for step in range(1, n_tp):
        source = lax.rem(tp_index + n_tp - step, n_tp)
        part_copy(step, source).wait()
    for step, which in others:
        half_send(step, which).wait_send()
        half_pass(step, which, side).wait_send()
        half_pass(step, which, 1 - side).wait_recv()
    sibling_copy(tp_index).wait_send()
    sibling_copy(sibling).wait_recv()


def mixer(query_rows, key_rows, value_rows, output_weight):
    n_sp, n_tp = lax.axis_size("sp"), lax.axis_size("tp")
    shard_len, features = query_rows.shape
    tokens = shard_len // n_tp
    heads = features // HEAD_DIM
    in_vmem = pl.BlockSpec(memory_space=pltpu.VMEM)
    dma = pltpu.SemaphoreType.DMA
    parts, weights = pl.pallas_call(
        functools.partial(mixer_kernel, n_sp, n_tp),
        out_shape=(
            jax.ShapeDtypeStruct((n_tp, tokens, features), jnp.bfloat16),
            jax.ShapeDtypeStruct((n_tp,) + output_weight.shape, output_weight.dtype),
        ),
        in_specs=[in_vmem] * 4,
        out_specs=(in_vmem, in_vmem),
        scratch_shapes=[
            pltpu.VMEM((n_sp, 2, shard_len, features), jnp.bfloat16),
            pltpu.VMEM((shard_len, features), jnp.float32),
            pltpu.VMEM((heads, shard_len, KBLK), jnp.float32),
            pltpu.VMEM((n_tp, tokens, features), jnp.bfloat16),
            dma((n_sp, 2)),
            dma((n_sp, 2)),
            dma((n_tp,)),
            dma((n_tp,)),
            dma((n_tp,)),
            dma((n_tp,)),
            dma((n_tp,)),
            dma((n_tp,)),
            dma((3,)),
        ],
        compiler_params=pltpu.CompilerParams(collective_id=3, has_side_effects=True),
    )(query_rows, key_rows, value_rows, output_weight)
    by_token = jnp.concatenate([parts[index] for index in range(n_tp)], axis=1)
    return by_token, weights.reshape(-1, output_weight.shape[1])


def exchange_kernel(n_sp, n_tp, src, dst, send_sem, recv_sem, own_sem):
    count = n_sp * n_tp
    me = lax.axis_index("sp") * n_tp + lax.axis_index("tp")

    def place(peer):
        return {"sp": peer // n_tp, "tp": lax.rem(peer, n_tp)}

    def copy(step, peer, landing):
        return pltpu.make_async_remote_copy(
            src_ref=src.at[peer],
            dst_ref=dst.at[landing],
            send_sem=send_sem.at[step],
            recv_sem=recv_sem.at[step],
            device_id=place(peer),
            device_id_type=pl.DeviceIdType.MESH,
        )

    barrier = pltpu.get_barrier_semaphore()

    @pl.loop(1, count)
    def _(step):
        peer = lax.rem(me + step, count)
        pl.semaphore_signal(
            barrier, inc=1, device_id=place(peer), device_id_type=pl.DeviceIdType.MESH
        )

    pl.semaphore_wait(barrier, count - 1)
    own = pltpu.make_async_copy(src.at[me], dst.at[me], own_sem)
    own.start()

    @pl.loop(1, count)
    def _(step):
        copy(step, lax.rem(me + step, count), me).start()

    own.wait()

    @pl.loop(1, count)
    def _(step):
        copy(step, lax.rem(me + step, count), lax.rem(me + count - step, count)).wait()


def exchange(blocks, collective_id):
    n_sp, n_tp = lax.axis_size("sp"), lax.axis_size("tp")
    return pl.pallas_call(
        functools.partial(exchange_kernel, n_sp, n_tp),
        out_shape=jax.ShapeDtypeStruct(blocks.shape, blocks.dtype),
        in_specs=[pl.BlockSpec(memory_space=pl.ANY)],
        out_specs=pl.BlockSpec(memory_space=pl.ANY),
        scratch_shapes=[
            pltpu.SemaphoreType.DMA((n_sp * n_tp,)),
            pltpu.SemaphoreType.DMA((n_sp * n_tp,)),
            pltpu.SemaphoreType.DMA,
        ],
        compiler_params=pltpu.CompilerParams(
            collective_id=collective_id, has_side_effects=True
        ),
    )(blocks)


def local(
    query_rows,
    key_rows,
    value_rows,
    residual,
    output_weight,
    first_gain,
    first_bias,
    expert_ids,
    expert_share,
    gate_weight,
    up_weight,
    down_weight,
    shared_gate,
    shared_up,
    shared_down,
    second_gain,
    second_bias,
):
    by_token, weights = mixer(query_rows, key_rows, value_rows, output_weight)
    tokens_here = residual.shape[0]
    width = residual.shape[1]
    mixed = jnp.dot(by_token, weights, preferred_element_type=jnp.float32)
    normed = layer_norm(residual.astype(jnp.float32) + mixed, first_gain, first_bias).astype(
        jnp.bfloat16
    )
    top_count = expert_ids.shape[1]
    pair_count = tokens_here * top_count
    experts = lax.axis_size("sp") * lax.axis_size("tp")
    capacity = max(2, 3 * pair_count // (2 * experts))
    flat_ids = expert_ids.reshape(pair_count)
    one_hot = (flat_ids[:, None] == jnp.arange(experts, dtype=jnp.int32)[None, :]).astype(
        jnp.bfloat16
    )
    earlier_mask = (jnp.arange(pair_count)[:, None] > jnp.arange(pair_count)[None, :]).astype(
        jnp.bfloat16
    )
    before = jnp.dot(earlier_mask, one_hot, preferred_element_type=jnp.float32)
    ranked = jnp.sum(before * one_hot, axis=1).astype(jnp.int32)
    slot_ids = flat_ids * capacity + ranked
    selector = jnp.any(
        slot_ids.reshape(tokens_here, top_count)[None, :, :]
        == jnp.arange(experts * capacity, dtype=jnp.int32)[:, None, None],
        axis=2,
    )
    outgoing = jnp.dot(selector.astype(jnp.bfloat16), normed, preferred_element_type=jnp.float32)
    outgoing = outgoing.astype(jnp.bfloat16).reshape(experts, capacity, width)
    slot_rows = exchange(outgoing, 1)
    flat_rows = slot_rows.reshape(-1, width)
    gate_act = jnp.dot(flat_rows, gate_weight[0], preferred_element_type=jnp.float32)
    up_act = jnp.dot(flat_rows, up_weight[0], preferred_element_type=jnp.float32)
    hidden = (jax.nn.silu(gate_act) * up_act).astype(jnp.bfloat16)
    produced = jnp.dot(hidden, down_weight[0], preferred_element_type=jnp.float32).astype(
        jnp.bfloat16
    )
    results = produced.reshape(slot_rows.shape)
    returned = lax.all_to_all(results, ("sp", "tp"), split_axis=0, concat_axis=0, tiled=True)
    flat_back = returned.reshape(experts * capacity, width)
    placed = slot_ids.reshape(tokens_here, top_count)[:, :, None] == jnp.arange(
        experts * capacity, dtype=jnp.int32
    )
    shares = jnp.sum(jnp.where(placed, expert_share[:, :, None], 0.0), axis=1)
    upper_part = lax.reduce_precision(shares, 8, 7)
    both = jnp.concatenate([upper_part, shares - upper_part], axis=0).astype(jnp.bfloat16)
    both_out = jnp.dot(both, flat_back, preferred_element_type=jnp.float32)
    routed = both_out[:tokens_here] + both_out[tokens_here:]
    gate_act = jnp.dot(normed, shared_gate, preferred_element_type=jnp.float32)
    up_act = jnp.dot(normed, shared_up, preferred_element_type=jnp.float32)
    shared_hidden = (jax.nn.silu(gate_act) * up_act).astype(jnp.bfloat16)
    shared_out = lax.optimization_barrier(
        jnp.dot(shared_hidden, shared_down, preferred_element_type=jnp.float32)
    )
    final = layer_norm(normed.astype(jnp.float32) + routed + shared_out, second_gain, second_bias)
    return final.astype(jnp.bfloat16)


def solution(mesh):
    return jax.shard_map(
        local,
        mesh=mesh,
        in_specs=(
            P(("grp", "sp"), "tp"),
            P(("grp", "sp"), "tp"),
            P(("grp", "sp"), "tp"),
            P(("grp", "sp", "tp"), None),
            P("tp", None),
            P(),
            P(),
            P(("grp", "sp", "tp"), None),
            P(("grp", "sp", "tp"), None),
            P(("sp", "tp"), None, None),
            P(("sp", "tp"), None, None),
            P(("sp", "tp"), None, None),
            P(),
            P(),
            P(),
            P(),
            P(),
        ),
        out_specs=P(("grp", "sp", "tp"), None),
        check_vma=False,
    )
```

```python
import functools

import jax
import jax.numpy as jnp
from jax import lax
from jax.experimental import pallas as pl
from jax.experimental.pallas import tpu as pltpu
from jax.sharding import PartitionSpec as P

HEAD_DIM = 128
KBLK = 128


NORM_EPS = 1e-05


def layer_norm(summed, gains, offset):
    average = jnp.mean(summed, axis=-1, keepdims=True)
    centred = summed - average
    spread = jnp.mean(centred * centred, axis=-1, keepdims=True)
    return centred * lax.rsqrt(spread + NORM_EPS) * gains + offset


def three_parts(exact):
    high = exact.astype(jnp.bfloat16)
    rest = exact - high.astype(jnp.float32)
    middle = rest.astype(jnp.bfloat16)
    low = (rest - middle.astype(jnp.float32)).astype(jnp.bfloat16)
    return jnp.concatenate([high, middle, low], axis=1)


def mixer_kernel(
    n_sp,
    n_tp,
    query_ref,
    key_ref,
    value_ref,
    weight_ref,
    parts_ref,
    weights_ref,
    held,
    summed,
    behind,
    ready,
    held_send,
    held_recv,
    weight_send,
    weight_recv,
    part_send,
    part_recv,
    pass_send,
    pass_recv,
    own_sem,
):
    mesh_ids = pl.DeviceIdType.MESH
    seq_index, tp_index = lax.axis_index("sp"), lax.axis_index("tp")
    shard_len, features = query_ref.shape
    tokens = shard_len // n_tp
    heads = features // HEAD_DIM
    tile = min(shard_len, 256)
    scale = HEAD_DIM ** (-0.5)
    has_next, has_last = seq_index < n_sp - 1, seq_index > 0
    after, ahead = lax.rem(seq_index + 1, n_sp), lax.rem(seq_index + n_sp - 1, n_sp)

    barrier = pltpu.get_barrier_semaphore()

    @pl.when(has_next)
    def _():
        pl.semaphore_signal(barrier, inc=1, device_id={"sp": after}, device_id_type=mesh_ids)

    @pl.when(has_last)
    def _():
        pl.semaphore_signal(barrier, inc=1, device_id={"sp": ahead}, device_id_type=mesh_ids)

    for step in range(1, n_tp):
        peer = lax.rem(tp_index + step, n_tp)
        pl.semaphore_signal(barrier, inc=1, device_id={"tp": peer}, device_id_type=mesh_ids)

    own_copies = [
        pltpu.make_async_copy(key_ref, held.at[seq_index, 0], own_sem.at[0]),
        pltpu.make_async_copy(value_ref, held.at[seq_index, 1], own_sem.at[1]),
        pltpu.make_async_copy(weight_ref, weights_ref.at[tp_index], own_sem.at[2]),
    ]
    for copy in own_copies:
        copy.start()
    summed[...] = jnp.zeros_like(summed)
    behind[...] = jnp.zeros_like(behind)
    pl.semaphore_wait(
        barrier, n_tp - 1 + has_next.astype(jnp.int32) + has_last.astype(jnp.int32)
    )

    def held_copy(step, which):
        block = lax.rem(seq_index - step + n_sp, n_sp)
        return pltpu.make_async_remote_copy(
            src_ref=held.at[block, which],
            dst_ref=held.at[block, which],
            send_sem=held_send.at[step, which],
            recv_sem=held_recv.at[step, which],
            device_id={"sp": after},
            device_id_type=mesh_ids,
        )

    def arrived(step, which):
        block = lax.rem(seq_index - step + n_sp, n_sp)
        return pltpu.make_async_remote_copy(
            src_ref=held.at[block, which],
            dst_ref=held.at[block, which],
            send_sem=held_send.at[step - 1, which],
            recv_sem=held_recv.at[step - 1, which],
            device_id={"sp": after},
            device_id_type=mesh_ids,
        )

    pair, side = tp_index // 2, lax.rem(tp_index, 2)
    pairs = n_tp // 2
    half = weight_ref.shape[0] // 2
    sibling = tp_index + 1 - 2 * side

    def sibling_copy(landing):
        return pltpu.make_async_remote_copy(
            src_ref=weight_ref,
            dst_ref=weights_ref.at[landing],
            send_sem=weight_send.at[0],
            recv_sem=weight_recv.at[0],
            device_id={"tp": sibling},
            device_id_type=mesh_ids,
        )

    def half_rows(which):
        return pl.ds(pl.multiple_of(which * half, half), half)

    def slot(step, which):
        return 1 + (step - 1) * 2 + which

    def half_send(step, which):
        target = lax.rem(pair + step, pairs) * 2 + which
        return pltpu.make_async_remote_copy(
            src_ref=weight_ref.at[half_rows(which)],
            dst_ref=weights_ref.at[tp_index, half_rows(which)],
            send_sem=weight_send.at[slot(step, which)],
            recv_sem=weight_recv.at[slot(step, side)],
            device_id={"tp": target},
            device_id_type=mesh_ids,
        )

    def half_arrived(step, which):
        source = lax.rem(pair + pairs - step, pairs) * 2 + which
        place = weights_ref.at[source, half_rows(side)]
        return pltpu.make_async_remote_copy(
            src_ref=place,
            dst_ref=place,
            send_sem=weight_send.at[slot(step, which)],
            recv_sem=weight_recv.at[slot(step, which)],
            device_id={"tp": source},
            device_id_type=mesh_ids,
        )

    def half_pass(step, which, part):
        source = lax.rem(pair + pairs - step, pairs) * 2 + which
        place = weights_ref.at[source, half_rows(part)]
        return pltpu.make_async_remote_copy(
            src_ref=place,
            dst_ref=place,
            send_sem=pass_send.at[slot(step, which)],
            recv_sem=pass_recv.at[slot(step, which)],
            device_id={"tp": sibling},
            device_id_type=mesh_ids,
        )

    others = [(step, which) for step in range(1, pairs) for which in range(2)]

    def part_copy(step, landing):
        peer = lax.rem(tp_index + step, n_tp)
        return pltpu.make_async_remote_copy(
            src_ref=ready.at[peer],
            dst_ref=parts_ref.at[landing],
            send_sem=part_send.at[step],
            recv_sem=part_recv.at[step],
            device_id={"tp": peer},
            device_id_type=mesh_ids,
        )

    for copy in own_copies:
        copy.wait()

    @pl.when(has_next)
    def _():
        for which in range(2):
            held_copy(0, which).start()

    for step, which in others:
        half_send(step, which).start()
    sibling_copy(tp_index).start()

    key_lane = lax.broadcasted_iota(jnp.int32, (tile, KBLK), 1)
    query_row = lax.broadcasted_iota(jnp.int32, (tile, KBLK), 0)
    from_row = lax.broadcasted_iota(jnp.int32, (KBLK, 2 * KBLK), 0)
    to_lane = lax.broadcasted_iota(jnp.int32, (KBLK, 2 * KBLK), 1)
    reach = ((from_row >= to_lane) | (to_lane >= KBLK)).astype(jnp.float32).astype(jnp.bfloat16)
    reach = jnp.concatenate([reach, reach, reach], axis=0)

    def visit(block, diagonal):
        for head in range(heads):
            lanes = slice(head * HEAD_DIM, (head + 1) * HEAD_DIM)
            for first_key in reversed(range(0, shard_len, KBLK)):
                key_block = held[block, 0, first_key : first_key + KBLK, lanes]
                value_block = held[block, 1, first_key : first_key + KBLK, lanes]
                for first_query in range(0, shard_len, tile):
                    if diagonal and first_key >= first_query + tile:
                        continue
                    masked = diagonal and first_key + KBLK > first_query
                    rows = slice(first_query, first_query + tile)
                    score = scale * lax.dot_general(
                        query_ref[rows, lanes],
                        key_block,
                        (((1,), (1,)), ((), ())),
                        preferred_element_type=jnp.float32,
                    )
                    usable = (key_lane + first_key) < (query_row + first_query)
                    spent = jnp.maximum(score, 0.0) + jnp.log(1.0 + jnp.exp(-jnp.abs(score)))
                    if masked:
                        spent = jnp.where(usable, spent, 0.0)
                    sums = jnp.dot(three_parts(spent), reach, preferred_element_type=jnp.float32)
                    share = jnp.exp(score - sums[:, :KBLK])
                    if masked:
                        share = jnp.where(usable, share, 0.0)
                    piece = jnp.dot(
                        share.astype(jnp.bfloat16),
                        value_block,
                        preferred_element_type=jnp.float32,
                    )
                    before = behind[head, rows, :]
                    summed[rows, lanes] += piece * jnp.exp(-before)
                    behind[head, rows, :] = before + sums[:, KBLK:]

    visit(seq_index, True)

    @pl.loop(1, seq_index + 1)
    def _(step):
        for which in range(2):
            arrived(step, which).wait_recv()

        @pl.when(has_next)
        def _():
            for which in range(2):
                held_copy(step, which).start()

        visit(seq_index - step, False)

    for peer in range(n_tp):
        ready[peer] = summed[peer * tokens : (peer + 1) * tokens, :].astype(jnp.bfloat16)
    for step in range(1, n_tp):
        part_copy(step, tp_index).start()
    parts_ref[tp_index] = ready[tp_index]
    for step, which in others:
        half_arrived(step, which).wait_recv()
        half_pass(step, which, side).start()

    @pl.when(has_next)
    def _():
        @pl.loop(0, seq_index + 1)
        def _(step):
            for which in range(2):
                held_copy(step, which).wait_send()

    for step in range(1, n_tp):
        source = lax.rem(tp_index + n_tp - step, n_tp)
        part_copy(step, source).wait()
    for step, which in others:
        half_send(step, which).wait_send()
        half_pass(step, which, side).wait_send()
        half_pass(step, which, 1 - side).wait_recv()
    sibling_copy(tp_index).wait_send()
    sibling_copy(sibling).wait_recv()


def mixer(query_rows, key_rows, value_rows, output_weight):
    n_sp, n_tp = lax.axis_size("sp"), lax.axis_size("tp")
    shard_len, features = query_rows.shape
    tokens = shard_len // n_tp
    heads = features // HEAD_DIM
    in_vmem = pl.BlockSpec(memory_space=pltpu.VMEM)
    dma = pltpu.SemaphoreType.DMA
    parts, weights = pl.pallas_call(
        functools.partial(mixer_kernel, n_sp, n_tp),
        out_shape=(
            jax.ShapeDtypeStruct((n_tp, tokens, features), jnp.bfloat16),
            jax.ShapeDtypeStruct((n_tp,) + output_weight.shape, output_weight.dtype),
        ),
        in_specs=[in_vmem] * 4,
        out_specs=(in_vmem, in_vmem),
        scratch_shapes=[
            pltpu.VMEM((n_sp, 2, shard_len, features), jnp.bfloat16),
            pltpu.VMEM((shard_len, features), jnp.float32),
            pltpu.VMEM((heads, shard_len, KBLK), jnp.float32),
            pltpu.VMEM((n_tp, tokens, features), jnp.bfloat16),
            dma((n_sp, 2)),
            dma((n_sp, 2)),
            dma((n_tp,)),
            dma((n_tp,)),
            dma((n_tp,)),
            dma((n_tp,)),
            dma((n_tp,)),
            dma((n_tp,)),
            dma((3,)),
        ],
        compiler_params=pltpu.CompilerParams(collective_id=3, has_side_effects=True),
    )(query_rows, key_rows, value_rows, output_weight)
    by_token = jnp.concatenate([parts[index] for index in range(n_tp)], axis=1)
    return by_token, weights.reshape(-1, output_weight.shape[1])


def exchange_kernel(n_sp, n_tp, src, dst, send_sem, recv_sem, own_sem):
    count = n_sp * n_tp
    me = lax.axis_index("sp") * n_tp + lax.axis_index("tp")

    def place(peer):
        return {"sp": peer // n_tp, "tp": lax.rem(peer, n_tp)}

    def copy(step, peer, landing):
        return pltpu.make_async_remote_copy(
            src_ref=src.at[peer],
            dst_ref=dst.at[landing],
            send_sem=send_sem.at[step],
            recv_sem=recv_sem.at[step],
            device_id=place(peer),
            device_id_type=pl.DeviceIdType.MESH,
        )

    barrier = pltpu.get_barrier_semaphore()

    @pl.loop(1, count)
    def _(step):
        peer = lax.rem(me + step, count)
        pl.semaphore_signal(
            barrier, inc=1, device_id=place(peer), device_id_type=pl.DeviceIdType.MESH
        )

    pl.semaphore_wait(barrier, count - 1)
    own = pltpu.make_async_copy(src.at[me], dst.at[me], own_sem)
    own.start()

    @pl.loop(1, count)
    def _(step):
        copy(step, lax.rem(me + step, count), me).start()

    own.wait()

    @pl.loop(1, count)
    def _(step):
        copy(step, lax.rem(me + step, count), lax.rem(me + count - step, count)).wait()


def exchange(blocks, collective_id):
    n_sp, n_tp = lax.axis_size("sp"), lax.axis_size("tp")
    return pl.pallas_call(
        functools.partial(exchange_kernel, n_sp, n_tp),
        out_shape=jax.ShapeDtypeStruct(blocks.shape, blocks.dtype),
        in_specs=[pl.BlockSpec(memory_space=pl.ANY)],
        out_specs=pl.BlockSpec(memory_space=pl.ANY),
        scratch_shapes=[
            pltpu.SemaphoreType.DMA((n_sp * n_tp,)),
            pltpu.SemaphoreType.DMA((n_sp * n_tp,)),
            pltpu.SemaphoreType.DMA,
        ],
        compiler_params=pltpu.CompilerParams(
            collective_id=collective_id, has_side_effects=True
        ),
    )(blocks)


def local(
    query_rows,
    key_rows,
    value_rows,
    residual,
    output_weight,
    first_gain,
    first_bias,
    expert_ids,
    expert_share,
    gate_weight,
    up_weight,
    down_weight,
    shared_gate,
    shared_up,
    shared_down,
    second_gain,
    second_bias,
):
    by_token, weights = mixer(query_rows, key_rows, value_rows, output_weight)
    tokens_here = residual.shape[0]
    width = residual.shape[1]
    mixed = jnp.dot(by_token, weights, preferred_element_type=jnp.float32)
    normed = layer_norm(residual.astype(jnp.float32) + mixed, first_gain, first_bias).astype(
        jnp.bfloat16
    )
    top_count = expert_ids.shape[1]
    pair_count = tokens_here * top_count
    experts = lax.axis_size("sp") * lax.axis_size("tp")
    capacity = max(2, 3 * pair_count // (2 * experts))
    flat_ids = expert_ids.reshape(pair_count)
    one_hot = (flat_ids[:, None] == jnp.arange(experts, dtype=jnp.int32)[None, :]).astype(
        jnp.bfloat16
    )
    earlier_mask = (jnp.arange(pair_count)[:, None] > jnp.arange(pair_count)[None, :]).astype(
        jnp.bfloat16
    )
    before = jnp.dot(earlier_mask, one_hot, preferred_element_type=jnp.float32)
    ranked = jnp.sum(before * one_hot, axis=1).astype(jnp.int32)
    slot_ids = flat_ids * capacity + ranked
    selector = jnp.any(
        slot_ids.reshape(tokens_here, top_count)[None, :, :]
        == jnp.arange(experts * capacity, dtype=jnp.int32)[:, None, None],
        axis=2,
    )
    outgoing = jnp.dot(selector.astype(jnp.bfloat16), normed, preferred_element_type=jnp.float32)
    outgoing = outgoing.astype(jnp.bfloat16).reshape(experts, capacity, width)
    slot_rows = exchange(outgoing, 1)
    flat_rows = slot_rows.reshape(-1, width)
    gate_act = jnp.dot(flat_rows, gate_weight[0], preferred_element_type=jnp.float32)
    up_act = jnp.dot(flat_rows, up_weight[0], preferred_element_type=jnp.float32)
    hidden = (jax.nn.silu(gate_act) * up_act).astype(jnp.bfloat16)
    produced = jnp.dot(hidden, down_weight[0], preferred_element_type=jnp.float32).astype(
        jnp.bfloat16
    )
    results = produced.reshape(slot_rows.shape)
    returned = lax.all_to_all(results, ("sp", "tp"), split_axis=0, concat_axis=0, tiled=True)
    flat_back = returned.reshape(experts * capacity, width)
    placed = slot_ids.reshape(tokens_here, top_count)[:, :, None] == jnp.arange(
        experts * capacity, dtype=jnp.int32
    )
    shares = jnp.sum(jnp.where(placed, expert_share[:, :, None], 0.0), axis=1)
    upper_part = lax.reduce_precision(shares, 8, 7)
    both = jnp.concatenate([upper_part, shares - upper_part], axis=0).astype(jnp.bfloat16)
    both_out = jnp.dot(both, flat_back, preferred_element_type=jnp.float32)
    routed = both_out[:tokens_here] + both_out[tokens_here:]
    gate_act = jnp.dot(normed, shared_gate, preferred_element_type=jnp.float32)
    up_act = jnp.dot(normed, shared_up, preferred_element_type=jnp.float32)
    shared_hidden = (jax.nn.silu(gate_act) * up_act).astype(jnp.bfloat16)
    shared_out = lax.optimization_barrier(
        jnp.dot(shared_hidden, shared_down, preferred_element_type=jnp.float32)
    )
    final = layer_norm(normed.astype(jnp.float32) + routed + shared_out, second_gain, second_bias)
    return final.astype(jnp.bfloat16)


def solution(mesh):
    return jax.shard_map(
        local,
        mesh=mesh,
        in_specs=(
            P(("grp", "sp"), "tp"),
            P(("grp", "sp"), "tp"),
            P(("grp", "sp"), "tp"),
            P(("grp", "sp", "tp"), None),
            P("tp", None),
            P(),
            P(),
            P(("grp", "sp", "tp"), None),
            P(("grp", "sp", "tp"), None),
            P(("sp", "tp"), None, None),
            P(("sp", "tp"), None, None),
            P(("sp", "tp"), None, None),
            P(),
            P(),
            P(),
            P(),
            P(),
        ),
        out_specs=P(("grp", "sp", "tp"), None),
        check_vma=False,
    )
```
